32 devices in a mesh: ep: 4 (over y, x), tp: 8 (over z, core).
Axes of the slice: x: 2, y: 2, z: 4, core: 2. Of those that a mesh axis runs over, the one named last changes fastest.
Arguments:
- queries: bfloat16 [4096, 1024], P('ep', 'tp'), may hold values from -12 to 12
- keys: bfloat16 [4096, 1024], P('ep', 'tp'), may hold values from -12 to 12
- values: bfloat16 [4096, 2048], P('ep', 'tp'), may hold values from -6 to 6
- out_gate: bfloat16 [4096, 2048], P('ep', 'tp'), may hold values from -6 to 6
- in_gate: float32 [16, 4096], P('tp', 'ep'), may hold values from -8 to 100
- forget_gate: float32 [16, 4096], P('tp', 'ep'), may hold values from 0 to 16
- out_gain: float32 [2048], P('tp'), may hold values from 0.1 to 1.9
- out_weight: bfloat16 [2048, 4096], P('tp'), may hold values from -0.1875 to 0.1875
- moe_rows: bfloat16 [512, 4096], P('ep'), may hold values from -36 to 36
- moe_gain: float32 [4096], replicated, may hold values from 0.1 to 1.9
- routes: int32 [512, 2], P('ep'), may hold values from 0 to 3, all different within a row; in each aligned block of 128 rows (0 to 127, 128 to 255, ...) at most 96 rows name the same one
- route_weight: float32 [512, 2], P('ep'), may hold values from 0.2 to 1.2
- expert_gate: bfloat16 [4, 4096, 4096], P('ep', None, 'tp'), may hold values from -0.09375 to 0.09375
- expert_up: bfloat16 [4, 4096, 4096], P('ep', None, 'tp'), may hold values from -0.09375 to 0.09375
- expert_down: bfloat16 [4, 4096, 4096], P('ep', 'tp'), may hold values from -0.125 to 0.125
- shared_gate: bfloat16 [4096, 2048], P(None, 'tp'), may hold values from -0.09375 to 0.09375
- shared_up: bfloat16 [4096, 2048], P(None, 'tp'), may hold values from -0.09375 to 0.09375
- shared_down: bfloat16 [2048, 4096], P('tp'), may hold values from -0.1875 to 0.1875
Outputs:
- mixer_out: bfloat16 [4096, 4096], P('ep', 'tp')
- moe_out: bfloat16 [512, 4096], P('ep', 'tp')
The draws below stay inside these ranges and needn't reach their ends.
Inputs may be any that keep to these rules, and one draw needn't show every extreme that they name: `routes`: each row names 2 different experts. Within the 128 rows of one index of ep no expert is named more than 96 times, a bound that some block reaches.
All inputs are finite; a program needn't handle non-finite values.
Results may differ from the reference program's by a relative error of at most 0.019.
Values may be sent and summed in bfloat16 or wider, within the bound.
A program may use at most 128 MiB of HBM per device.

```python
import math
import jax
import jax.numpy as jnp
import numpy as np
from jax import lax

D = 4096
CELL_HEADS = 16
DK = 64
DV = 128
BLK = 64
TA_DEV = 1024
FE = 4096
FS = 2048
TOPK = 2
TB_DEV = 128
HW = 2048
SEQUENCE_TOKENS = 4096
TOKB = 512
EXPERTS = 4
CAP = 96
N_EP = 4
N_TP = 8


def draw_forget_gate(key, part):
    split_random_keys = jax.random.split(jax.random.fold_in(key, 11), 7)
    slow_share = 0.5
    slow_head = jax.random.bernoulli(split_random_keys[0], slow_share, (CELL_HEADS, 1))
    token_position = jnp.arange(SEQUENCE_TOKENS)
    slow_total = jnp.exp(jax.random.uniform(split_random_keys[1], (CELL_HEADS, 1), minval=jnp.log(0.15), maxval=jnp.log(0.5)))
    slow_rate = slow_total / SEQUENCE_TOKENS
    fast_rate = 1.0 / jnp.exp(jax.random.uniform(split_random_keys[2], (CELL_HEADS, 1), minval=jnp.log(20.0), maxval=jnp.log(60.0)))
    forget_decay_speed = jnp.where(slow_head, slow_rate, fast_rate)
    owner = token_position // TA_DEV
    jitter = jnp.exp(jax.random.uniform(split_random_keys[3], (CELL_HEADS, SEQUENCE_TOKENS // TA_DEV), minval=-0.2, maxval=0.2))
    device_factor = (2.0 ** (owner % 2).astype(jnp.float32))[None, :] * jnp.take(jitter, owner, axis=1)
    noise = jnp.exp(jax.random.uniform(split_random_keys[4], (CELL_HEADS, SEQUENCE_TOKENS), minval=-0.5, maxval=0.5))
    forget_decay_speed = forget_decay_speed * device_factor * noise
    spike_location = jax.random.randint(split_random_keys[5], (CELL_HEADS, 2, 1), 0, SEQUENCE_TOKENS)
    spike_reached = jnp.any(token_position[None, None, :] == spike_location, axis=1)
    spike_penalty = jax.random.uniform(split_random_keys[6], (CELL_HEADS, SEQUENCE_TOKENS), minval=0.2, maxval=0.45)
    forget_decay_speed = jnp.where(spike_reached, -jnp.log(1.0 - spike_penalty), forget_decay_speed)
    return (-jnp.log(jnp.expm1(forget_decay_speed))).astype(jnp.float32)


def draw_in_gate(key, part):
    split_random_keys = jax.random.split(jax.random.fold_in(key, 23), 2)
    return jnp.clip(1.5 * jax.random.normal(split_random_keys[1], (CELL_HEADS, SEQUENCE_TOKENS)), -8.0, 8.0).astype(jnp.float32)


def draw_moe_rows(key, part):
    split_random_keys = jax.random.split(jax.random.fold_in(key, 37), 3)
    row_scale = jnp.exp(jax.random.uniform(split_random_keys[0], (TOKB, 1), minval=jnp.log(0.3), maxval=jnp.log(3.0)))
    col_scale = jnp.exp(jax.random.uniform(split_random_keys[1], (1, D), minval=jnp.log(0.5), maxval=jnp.log(2.0)))
    base_draw = jax.random.normal(split_random_keys[2], (TOKB, D))
    return (jnp.clip(base_draw, -6.0, 6.0) * row_scale * col_scale).astype(jnp.bfloat16)


def common_direction(key):
    base = jax.random.normal(jax.random.fold_in(key, 51), (CELL_HEADS, DK))
    unit = base / jnp.sqrt(jnp.sum(base * base, axis=1, keepdims=True))
    return (8.0 * unit).reshape(1, CELL_HEADS * DK)


def draw_queries(key, part):
    noise_key = jax.random.fold_in(key, 61)
    noise = jnp.clip(jax.random.normal(noise_key, (SEQUENCE_TOKENS, CELL_HEADS * DK)), -4.0, 4.0)
    return (noise + common_direction(key)).astype(jnp.bfloat16)


def draw_keys(key, part):
    noise_key = jax.random.fold_in(key, 71)
    noise = jnp.clip(jax.random.normal(noise_key, (SEQUENCE_TOKENS, CELL_HEADS * DK)), -4.0, 4.0)
    return (noise + common_direction(key)).astype(jnp.bfloat16)


def strengthened(drawn, key, source, target, shards_of, factor):
    owner, partner = [(jnp.arange(drawn.shape[axis_at]) // (drawn.shape[axis_at] // shards_of)).reshape([-1 if axis == axis_at else 1 for axis in range(drawn.ndim)]) for axis_at in (source, target)]
    chosen = jax.random.permutation(key, shards_of)[partner]
    strong = (owner == chosen) | (owner == (partner + shards_of // 2) % shards_of)
    return jnp.where(strong, factor * drawn, drawn)


def block_levels(rng, dims, shards, low, high):
    def one(axis_at, parts):
        heights = jax.random.uniform(jax.random.fold_in(jax.random.fold_in(rng, 6), axis_at), (parts,), jnp.float32, low / len(shards), high / len(shards))
        return jnp.repeat(jnp.exp(heights), dims[axis_at] // parts).reshape((-1,) + (1,) * (len(dims) - axis_at - 1))

    level = one(*shards[0])
    for cut in shards[1:]:
        level = level * one(*cut)
    return level


def shared_out(own_key, own, number, rows, count, top, reach, slope):
    ranking = jax.random.permutation(own_key, count)
    crowded, common = portions_of(count, rows * top, reach, slope, True), portions_of(count, rows * top, reach, slope, False)
    places = jnp.arange(count)

    def named(tallies, rotation):
        used = int((tallies > 0).sum())
        fixed = max(1, used // 4)
        shifted = fixed + (places - fixed + rotation * (used - fixed)) % max(1, count - fixed)
        return jnp.zeros((count,), jnp.int32).at[ranking[jnp.where(places < fixed, places, shifted)]].set(jnp.asarray(tallies, jnp.int32))

    tallies = jnp.where(number % 4 == 0, named(crowded, number // 4), named(common, number - number // 4 - 1))
    mixed = jax.random.permutation(jax.random.fold_in(own, 3), count)
    source_of, taker = mixed[0:count // 2 * 2:2], mixed[1:count // 2 * 2:2]
    room = jnp.minimum(tallies[source_of] - 1, reach - tallies[taker]) // 2
    room = jnp.where((source_of == ranking[0]) | (taker == ranking[0]) | (tallies[taker] == 0), 0, jnp.maximum(room, 0))
    shifted = jax.random.randint(jax.random.fold_in(own, 4), (count // 2,), 0, 1 << 20) % (room + 1)
    tallies = tallies.at[source_of].add(-shifted).at[taker].add(shifted)
    labels = jnp.searchsorted(jnp.cumsum(tallies), jnp.arange(rows * top), side="right").astype(jnp.int32)
    table = labels.reshape(top, rows).T
    table = table[jax.random.permutation(jax.random.fold_in(own, 1), rows)]
    rotation = jax.random.randint(jax.random.fold_in(own, 2), (rows, 1), 0, top)
    return jnp.take_along_axis(table, (jnp.arange(top)[None, :] + rotation) % top, axis=1)


def portions_of(amount, total, bound, skew, full):
    weights = [(1 << 20) // math.isqrt(standing ** skew) + 1 for standing in range(1, amount + 1)]
    largest = bound if full else min(bound, max(-(-total // amount), total * weights[0] // sum(weights)))
    least = 1 if total - largest >= amount - 1 else 0
    counts, rest = [largest] + [least] * (amount - 1), total - largest - least * (amount - 1)
    while rest > 0:
        movable = [i for i in range(1, amount) if counts[i] < largest] or [i for i in range(1, amount) if counts[i] < bound]
        mass, remaining = sum([weights[i] for i in movable]), rest
        for i in movable:
            extra = min(bound - counts[i], max(1, remaining * weights[i] // mass), rest)
            counts[i] = counts[i] + extra
            rest = rest - extra
    return np.array(counts)


def centred(rng, shape, spread, bound, cuts=(), kind=jnp.bfloat16):
    loudness = block_levels(rng, shape, cuts, -0.22, 0.18) if cuts else 1.0
    result = jax.random.normal(rng, shape, jnp.float32) * spread * loudness
    return jnp.minimum(jnp.maximum(result, -bound), bound).astype(kind)


def heavy_noise(rng, extent, width, bound, shards, heavy, kind=jnp.bfloat16):
    values = width * jax.random.normal(rng, extent, jnp.float32)
    if shards:
        values = values * block_levels(rng, extent, shards, -0.22, 0.18)
    return jnp.clip(strengthened(values, jax.random.fold_in(rng, 3), *heavy), -bound, bound).astype(kind)


def setup_inputs(seed: int = 0) -> dict:
    arg_keys = jax.random.split(jax.random.key(seed), 19)
    queries = draw_queries(jax.random.fold_in(arg_keys[18], 71), 0)
    keys = draw_keys(jax.random.fold_in(arg_keys[18], 71), 0)
    values = centred(arg_keys[2], (SEQUENCE_TOKENS, HW), 1.0, 6.0, ((0, 4), (1, 8)))
    out_gate = centred(arg_keys[3], (SEQUENCE_TOKENS, HW), 1.0, 6.0, ((0, 4), (1, 8)))
    in_gate = draw_in_gate(jax.random.fold_in(arg_keys[18], 71), 0)
    forget_gate = draw_forget_gate(jax.random.fold_in(arg_keys[18], 71), 0)
    out_gain = jnp.clip(1.0 + 0.18 * jax.random.normal(arg_keys[6], (HW,), jnp.float32), 0.1, 1.9)
    out_weight = heavy_noise(arg_keys[7], (HW, D), HW ** -0.5, 0.1875, ((0, 8),), (0, 1, 8, 2.0))
    moe_rows = draw_moe_rows(jax.random.fold_in(arg_keys[18], 71), 0)
    moe_gain = jnp.clip(1.0 + 0.18 * jax.random.normal(arg_keys[9], (D,), jnp.float32), 0.1, 1.9)
    routes_keys = jax.random.split(jax.random.fold_in(arg_keys[10], 1), TOKB // TB_DEV)
    routes_turns = jax.random.permutation(jax.random.fold_in(arg_keys[10], 3), TOKB // TB_DEV)
    routes = jax.vmap(lambda own, number: shared_out(jax.random.fold_in(arg_keys[10], 2), own, number, TB_DEV, EXPERTS, TOPK, CAP, 2))(routes_keys, routes_turns).reshape((TOKB, TOPK))
    route_weight = jnp.clip(0.2 + 1 * jax.random.uniform(arg_keys[11], (TOKB, TOPK), jnp.float32) ** block_levels(arg_keys[11], (TOKB, TOPK), ((0, 4),), -0.2, 0.2), 0.2, 1.2)
    expert_gate = centred(arg_keys[12], (EXPERTS, D, FE), D ** -0.5, 0.09375, ((0, 4), (2, 8)))
    expert_up = centred(arg_keys[13], (EXPERTS, D, FE), D ** -0.5, 0.09375, ((0, 4), (2, 8)))
    expert_down = heavy_noise(arg_keys[14], (EXPERTS, FE, D), FE ** -0.5, 0.125, ((0, 4), (1, 8)), (1, 2, 8, 2.0))
    shared_gate = centred(arg_keys[15], (D, FS), D ** -0.5, 0.09375, ((1, 8),))
    shared_up = centred(arg_keys[16], (D, FS), D ** -0.5, 0.09375, ((1, 8),))
    shared_down = heavy_noise(arg_keys[17], (FS, D), FS ** -0.5, 0.1875, ((0, 8),), (0, 1, 8, 2.0))
    return {"queries": queries, "keys": keys, "values": values, "out_gate": out_gate, "in_gate": in_gate, "forget_gate": forget_gate, "out_gain": out_gain, "out_weight": out_weight, "moe_rows": moe_rows, "moe_gain": moe_gain, "routes": routes, "route_weight": route_weight, "expert_gate": expert_gate, "expert_up": expert_up, "expert_down": expert_down, "shared_gate": shared_gate, "shared_up": shared_up, "shared_down": shared_down}


highest = lax.Precision.HIGHEST

def group_sum(left_op, right_op, groups):
    group_width = left_op.shape[1] // groups

    def add_group(group_index, running):
        first = (group_index * group_width).astype(jnp.int32)
        left_part = lax.dynamic_slice_in_dim(left_op, first, group_width, 1)
        right_part = lax.dynamic_slice_in_dim(right_op, first, group_width, 0)
        product = jnp.dot(left_part, right_part, preferred_element_type=jnp.float32)
        rounded = lax.optimization_barrier(product.astype(jnp.bfloat16))
        return running + rounded.astype(jnp.float32)
    start_sum = jnp.zeros((left_op.shape[0], right_op.shape[1]), jnp.float32)
    return lax.fori_loop(0, groups, add_group, start_sum)

def memory_head(inputs):
    query_head, key_head, value_head, gate_in, log_forget = inputs
    block_count = query_head.shape[0] // BLK
    scaled_query = (query_head * DK ** (-0.5)).reshape(block_count, BLK, DK)
    key_blocks = key_head.reshape(block_count, BLK, DK)
    value_blocks = value_head.reshape(block_count, BLK, DV)
    gate_blocks = gate_in.reshape(block_count, BLK)
    forget_blocks = log_forget.reshape(block_count, BLK)
    causal = jnp.tril(jnp.ones((BLK, BLK), dtype=bool))

    def block_step(state, block_inputs):
        matrix, normal_vec, stab = state
        query_b, key_b, value_b, gate_b, forget_b = block_inputs
        cumulative = jnp.cumsum(forget_b)
        intra = jnp.where(causal, cumulative[:, None] - cumulative[None, :] + gate_b[None, :], -jnp.inf)
        inter = cumulative + stab
        stab_t = jnp.maximum(inter, lax.optimization_barrier(jnp.max(intra, axis=1)))
        scores = jnp.dot(query_b, key_b.T, precision=highest) * jnp.exp(intra - stab_t[:, None])
        scores_low = lax.optimization_barrier(scores.astype(jnp.bfloat16)).astype(jnp.float32)
        inter_weight = jnp.exp(inter - stab_t)
        numer = jnp.dot(scores_low, value_b, precision=highest)
        numer = numer + inter_weight[:, None] * jnp.dot(query_b, matrix.T, precision=highest)
        signed = lax.optimization_barrier(jnp.sum(scores, axis=1)) + inter_weight * jnp.dot(query_b, normal_vec, precision=highest)
        cells = numer / jnp.maximum(jnp.abs(signed), jnp.exp(-stab_t))[:, None]
        block_last = cumulative[-1]
        state_logs = block_last - cumulative + gate_b
        stab_new = jnp.maximum(block_last + stab, jnp.max(state_logs))
        state_weight = jnp.exp(state_logs - stab_new)
        carried = jnp.exp(block_last + stab - stab_new)
        matrix_new = carried * matrix + jnp.dot((value_b * state_weight[:, None]).T, key_b, precision=highest)
        normal_new = carried * normal_vec + jnp.dot(state_weight, key_b, precision=highest)
        return ((matrix_new, normal_new, stab_new), cells)
    start_state = (jnp.zeros((DV, DK), jnp.float32), jnp.zeros((DK,), jnp.float32), jnp.zeros((), jnp.float32))
    _, cells = lax.scan(block_step, start_state, (scaled_query, key_blocks, value_blocks, gate_blocks, forget_blocks))
    return cells.reshape(block_count * BLK, DV)

def reference(queries, keys, values, out_gate, in_gate, forget_gate, out_gain, out_weight, moe_rows, moe_gain, routes, route_weight, expert_gate, expert_up, expert_down, shared_gate, shared_up, shared_down):
    log_forget = jax.nn.log_sigmoid(forget_gate)
    query_heads = queries.astype(jnp.float32).reshape(SEQUENCE_TOKENS, CELL_HEADS, DK).transpose(1, 0, 2)
    key_heads = keys.astype(jnp.float32).reshape(SEQUENCE_TOKENS, CELL_HEADS, DK).transpose(1, 0, 2)
    value_heads = values.astype(jnp.float32).reshape(SEQUENCE_TOKENS, CELL_HEADS, DV).transpose(1, 0, 2)
    cells = lax.map(memory_head, (query_heads, key_heads, value_heads, in_gate, log_forget))
    cells = cells.transpose(1, 0, 2).reshape(SEQUENCE_TOKENS, HW)
    mixed = (cells * jax.nn.sigmoid(out_gate.astype(jnp.float32)) * out_gain).astype(jnp.bfloat16)
    mixer_out = group_sum(mixed, out_weight, N_TP).astype(jnp.bfloat16)
    rows_wide = moe_rows.astype(jnp.float32)
    inverse = lax.rsqrt(lax.optimization_barrier(jnp.mean(rows_wide * rows_wide, axis=1, keepdims=True)) + 1e-06)
    normed = (rows_wide * inverse * moe_gain).astype(jnp.bfloat16)
    flat_routes = routes.reshape(-1).astype(jnp.int32)
    assigned = flat_routes.shape[0]
    per_block = TB_DEV * TOPK
    onehot = (flat_routes[:, None] == jnp.arange(EXPERTS, dtype=jnp.int32)[None, :]).astype(jnp.int32)
    running = jnp.cumsum(onehot.reshape(N_EP, per_block, EXPERTS), axis=1).reshape(assigned, EXPERTS)
    token_position = lax.optimization_barrier(jnp.sum(running * onehot, axis=1)) - 1
    owner_block = jnp.arange(assigned, dtype=jnp.int32) // per_block
    slot_index = (flat_routes * (N_EP * CAP) + owner_block * CAP + token_position).astype(jnp.int32)
    token_of = jnp.arange(assigned, dtype=jnp.int32) // TOPK
    slot_table = jnp.zeros((EXPERTS * N_EP * CAP,), jnp.int32).at[slot_index].set(token_of)
    slot_table = slot_table.reshape(EXPERTS, N_EP * CAP)

    def expert_rows(inputs):
        row_ids, weight_gate, weight_up, weight_down = inputs
        chosen = normed[row_ids]
        gate_val = jnp.dot(chosen, weight_gate, preferred_element_type=jnp.float32)
        up_val = jnp.dot(chosen, weight_up, preferred_element_type=jnp.float32)
        hidden = (jax.nn.silu(gate_val) * up_val).astype(jnp.bfloat16)
        return group_sum(hidden, weight_down, N_TP).astype(jnp.bfloat16)
    results = lax.map(expert_rows, (slot_table, expert_gate, expert_up, expert_down))
    picked = results.reshape(EXPERTS * N_EP * CAP, D)[slot_index].astype(jnp.float32).reshape(TOKB, TOPK, D)
    shared_gate_val = jnp.dot(normed, shared_gate, preferred_element_type=jnp.float32)
    shared_up_val = jnp.dot(normed, shared_up, preferred_element_type=jnp.float32)
    shared_hidden = (jax.nn.silu(shared_gate_val) * shared_up_val).astype(jnp.bfloat16)
    shared_sum = group_sum(shared_hidden, shared_down, N_TP)
    moe_out = (lax.optimization_barrier(jnp.sum(picked * route_weight[:, :, None], axis=1)) + shared_sum).astype(jnp.bfloat16)
    return (mixer_out, moe_out)
```

```python
import functools

import jax
import jax.numpy as jnp
from jax import lax
from jax.experimental import pallas as pl
from jax.experimental.pallas import tpu as pltpu
from jax.sharding import PartitionSpec as P

DK = 64
DV = 128
CH = 128
F32 = jnp.float32
BF16 = jnp.bfloat16
VM = pl.BlockSpec(memory_space=pltpu.VMEM)


def gate_rows(ig, fg):
    lane = lax.broadcasted_iota(jnp.int32, ig.shape, 1)
    total = jnp.minimum(fg, 0.0) - jnp.log1p(jnp.exp(-jnp.abs(fg)))
    step = 1
    while step < CH:
        total = total + jnp.where(lane >= step, pltpu.roll(total, step, 1), 0.0)
        step *= 2
    level = ig - total
    top = level
    step = 1
    while step < CH:
        top = jnp.maximum(top, jnp.where(lane >= step, pltpu.roll(top, step, 1), -1e30))
        step *= 2
    return total, level, top


def columns_of(parts):
    rows = sum(part.shape[0] for part in parts)
    padded = -(-rows // 128) * 128
    if padded > rows:
        parts = list(parts) + [jnp.zeros((padded - rows, CH), F32)]
    return jnp.concatenate(parts, axis=0).T


def split_bf16(x):
    high = x.astype(BF16)
    return high, (x - high.astype(F32)).astype(BF16)


def weighted_keys(keys, cols, first, heads, chunks):
    lane_head = lax.broadcasted_iota(jnp.int32, keys.shape, 1) // DK
    weight = jnp.broadcast_to(cols[:, first : first + 1], keys.shape)
    for h in range(1, heads):
        at = first + h * chunks
        weight = jnp.where(lane_head == h, jnp.broadcast_to(cols[:, at : at + 1], keys.shape), weight)
    return split_bf16(keys.astype(F32) * weight)


def add_outer(kw, values):
    dims = (((0,), (0,)), ((), ()))
    return lax.dot_general(kw[0], values, dims, preferred_element_type=F32) + lax.dot_general(
        kw[1], values, dims, preferred_element_type=F32
    )


def pick_head(parts, shape, axis):
    head = lax.broadcasted_iota(jnp.int32, shape, axis) // DK
    out = jnp.broadcast_to(parts[0], shape)
    for h in range(1, len(parts)):
        out = jnp.where(head == h, jnp.broadcast_to(parts[h], shape), out)
    return out


def summary_kernel(heads, chunks, k_ref, v_ref, ig_ref, fg_ref, out_ref):
    width = heads * DK
    total, level, top = gate_rows(ig_ref[...], fg_ref[...])
    shape = total.shape
    chunk = lax.broadcasted_iota(jnp.int32, shape, 0) % chunks
    last = jnp.broadcast_to(total[:, CH - 1 : CH], shape)
    suffix = last
    step = 1
    while step < chunks:
        moved = pltpu.roll(suffix, shape[0] - step, 0)
        suffix = suffix + jnp.where(chunk + step < chunks, moved, 0.0)
        step *= 2
    reach = suffix + jnp.broadcast_to(top[:, CH - 1 : CH], shape)
    tops = [
        jnp.max(reach[h * chunks : (h + 1) * chunks], axis=0, keepdims=True) for h in range(heads)
    ]
    weight = [
        jnp.exp(
            level[h * chunks : (h + 1) * chunks] + suffix[h * chunks : (h + 1) * chunks] - tops[h]
        )
        for h in range(heads)
    ]
    cols = columns_of(weight)
    state = jnp.zeros((width, heads * DV + 128), F32)
    for c in range(chunks):
        rows = pl.ds(c * CH, CH)
        kw = weighted_keys(k_ref[rows, :], cols, c, heads, chunks)
        values = jnp.concatenate([v_ref[rows, :], jnp.ones((CH, 128), BF16)], axis=1)
        state = state + add_outer(kw, values)
    out_ref[...] = jnp.zeros_like(out_ref)
    out_ref[0:width, :] = pick_head(
        [state[:, h * DV : (h + 1) * DV] for h in range(heads)], (width, DV), 0
    )
    normal = state[:, heads * DV :].T
    out_ref[width : width + 1, 0:width] = normal[0:1, :]
    for h in range(heads):
        out_ref[width + 1 + h : width + 2 + h, :] = tops[h]
        at = width + 1 + heads + h
        out_ref[at : at + 1, :] = suffix[h * chunks : h * chunks + 1]


def cells_kernel(
    heads, chunks, pos_ref, q_ref, k_ref, v_ref, og_ref, ig_ref, fg_ref, gain_ref, sum_ref, out_ref
):
    width = heads * DK
    matrix = jnp.zeros((width, DV), F32)
    normal = jnp.zeros((1, width), F32)
    stab = [jnp.zeros((1, 128), F32) for _ in range(heads)]
    for e in range(sum_ref.shape[0]):
        reached = e < pos_ref[0]
        part = sum_ref.at[e]
        old_w, new_w, new_stab = [], [], []
        for h in range(heads):
            at = width + 1 + h
            carried = part[at + heads : at + heads + 1, :] + stab[h]
            there = part[at : at + 1, :]
            joined = jnp.maximum(carried, there)
            old_w.append(jnp.where(reached, jnp.exp(carried - joined), 1.0))
            new_w.append(jnp.where(reached, jnp.exp(there - joined), 0.0))
            new_stab.append(jnp.where(reached, joined, stab[h]))
        matrix = (
            pick_head(old_w, (width, DV), 0) * matrix
            + pick_head(new_w, (width, DV), 0) * part[0:width, :]
        )
        normal = (
            pick_head([w[:, 0:width] for w in old_w], (1, width), 1) * normal
            + pick_head([w[:, 0:width] for w in new_w], (1, width), 1)
            * part[width : width + 1, 0:width]
        )
        stab = new_stab
    normal_cols = jnp.broadcast_to(normal, (128, width)).T
    state = jnp.concatenate([matrix] * heads + [normal_cols], axis=1)

    total, level, top = gate_rows(ig_ref[...], fg_ref[...])
    shape = total.shape
    last = jnp.broadcast_to(total[:, CH - 1 : CH], shape)
    last_top = jnp.broadcast_to(top[:, CH - 1 : CH], shape)
    entering, leaving = [], []
    for h in range(heads):
        now = stab[h]
        for c in range(chunks):
            r = h * chunks + c
            entering.append(now)
            now = last[r : r + 1] + jnp.maximum(now, last_top[r : r + 1])
            leaving.append(now)
    entering = jnp.concatenate(entering, axis=0)
    leaving = jnp.concatenate(leaving, axis=0)
    peak = jnp.maximum(top, entering)
    decay = jnp.exp(last + entering - leaving)
    count = heads * chunks
    cols = columns_of(
        [
            peak,
            jnp.exp(entering - peak),
            jnp.exp(-(total + peak)),
            jnp.exp(last + level - leaving),
        ]
    )
    causal = lax.broadcasted_iota(jnp.int32, (CH, CH), 0) >= lax.broadcasted_iota(
        jnp.int32, (CH, CH), 1
    )
    lane_head = lax.broadcasted_iota(jnp.int32, (CH, width), 1) // DK
    for c in range(chunks):
        rows = pl.ds(c * CH, CH)
        keys = k_ref[rows, :]
        values = v_ref[rows, :]
        queries = q_ref[rows, :] * jnp.asarray(DK**-0.5, BF16)
        high, low = split_bf16(state)
        for h in range(heads):
            r = h * chunks + c
            mine = jnp.where(lane_head == h, queries, jnp.zeros_like(queries))
            raw = lax.dot_general(
                mine, keys, (((1,), (1,)), ((), ())), preferred_element_type=F32
            )
            logs = level[r : r + 1, :] - cols[:, r : r + 1]
            scores = raw * jnp.exp(jnp.where(causal, logs, -jnp.inf))
            inner = jnp.dot(
                scores.astype(BF16), values[:, h * DV : (h + 1) * DV], preferred_element_type=F32
            )
            across = 0.0
            for piece in (high, low):
                rhs = jnp.concatenate(
                    [piece[:, h * DV : (h + 1) * DV], piece[:, heads * DV :]], axis=1
                )
                across = across + jnp.dot(mine, rhs, preferred_element_type=F32)
            inter = cols[:, count + r : count + r + 1]
            signed = jnp.sum(scores, axis=1, keepdims=True) + inter * across[:, DV : DV + 1]
            divisor = jnp.maximum(jnp.abs(signed), cols[:, 2 * count + r : 2 * count + r + 1])
            cells = (inner + inter * across[:, :DV]) * (1.0 / divisor)
            at = slice(h * DV, (h + 1) * DV)
            gate = og_ref[rows, at].astype(F32)
            out_ref[rows, at] = (cells / (1.0 + jnp.exp(-gate)) * gain_ref[:, at]).astype(BF16)
        if c + 1 < chunks:
            kw = weighted_keys(keys, cols, 3 * count + c, heads, chunks)
            scale = pick_head(
                [decay[h * chunks + c : h * chunks + c + 1] for h in range(heads)], (width, 128), 0
            )
            rhs = jnp.concatenate([values, jnp.ones((CH, 128), BF16)], axis=1)
            state = state * jnp.concatenate([scale] * (heads + 1), axis=1) + add_outer(kw, rhs)


def mixed_cells(queries, keys, values, out_gate, in_gate, forget_gate, out_gain):
    tok_rows = queries.shape[0]
    heads = in_gate.shape[0]
    chunks = tok_rows // CH
    width = heads * DK
    ig = in_gate.reshape(heads * chunks, CH)
    fg = forget_gate.reshape(heads * chunks, CH)
    extra = -(-(1 + 2 * heads) // 8) * 8
    summary = pl.pallas_call(
        functools.partial(summary_kernel, heads, chunks),
        out_shape=jax.ShapeDtypeStruct((width + extra, 128), F32),
        in_specs=[VM] * 4,
        out_specs=VM,
        cost_estimate=pl.CostEstimate(flops=400_000_000, bytes_accessed=8_000_000, transcendentals=0),
    )(keys, values, ig, fg)
    everything = lax.all_gather(summary, "ep")
    pos = lax.axis_index("ep").astype(jnp.int32).reshape(1)
    return pl.pallas_call(
        functools.partial(cells_kernel, heads, chunks),
        out_shape=jax.ShapeDtypeStruct((tok_rows, heads * DV), BF16),
        in_specs=[pl.BlockSpec(memory_space=pltpu.SMEM)] + [VM] * 8,
        out_specs=VM,
        cost_estimate=pl.CostEstimate(flops=2_000_000_000, bytes_accessed=16_000_000, transcendentals=0),
    )(pos, queries, keys, values, out_gate, ig, fg, out_gain.reshape(1, -1), everything)


def mixer_kernel(a_ref, w_ref, out_ref):
    width = a_ref.shape[2]
    total = jnp.dot(a_ref[0], w_ref[0:width, :], preferred_element_type=F32)
    for i in range(1, a_ref.shape[0]):
        total = total + jnp.dot(
            a_ref[i], w_ref[i * width : (i + 1) * width, :], preferred_element_type=F32
        )
    out_ref[...] = total.astype(out_ref.dtype)


def mixer(gathered, weight):
    parts, rows, width = gathered.shape
    cols = weight.shape[1]
    tile = min(256, rows)
    return pl.pallas_call(
        mixer_kernel,
        grid=(rows // tile,),
        out_shape=jax.ShapeDtypeStruct((rows, cols), BF16),
        in_specs=[
            pl.BlockSpec((parts, tile, width), lambda r: (0, r, 0)),
            pl.BlockSpec((parts * width, cols), lambda r: (0, 0)),
        ],
        out_specs=pl.BlockSpec((tile, cols), lambda r: (r, 0)),
        cost_estimate=pl.CostEstimate(
            flops=2 * rows * parts * width * cols, bytes_accessed=8_000_000, transcendentals=0
        ),
    )(gathered, weight)


def hidden_kernel(x_ref, g_ref, u_ref, out_ref, gate_acc, up_acc):
    k = pl.program_id(0)
    x = x_ref[...]
    gate = jnp.dot(x, g_ref[...], preferred_element_type=F32)
    up = jnp.dot(x, u_ref[...], preferred_element_type=F32)

    @pl.when(k == 0)
    def _():
        gate_acc[...] = gate
        up_acc[...] = up

    @pl.when(k > 0)
    def _():
        gate_acc[...] += gate
        up_acc[...] += up

    @pl.when(k == pl.num_programs(0) - 1)
    def _():
        g = gate_acc[...]
        out_ref[...] = (g / (1.0 + jnp.exp(-g)) * up_acc[...]).astype(BF16)


def hidden_units(x, w_gate, w_up):
    rows, depth = x.shape
    cols = w_gate.shape[1]
    tile = min(512, depth)
    return pl.pallas_call(
        hidden_kernel,
        grid=(depth // tile,),
        out_shape=jax.ShapeDtypeStruct((rows, cols), BF16),
        in_specs=[
            pl.BlockSpec((rows, tile), lambda k: (0, k)),
            pl.BlockSpec((tile, cols), lambda k: (k, 0)),
            pl.BlockSpec((tile, cols), lambda k: (k, 0)),
        ],
        out_specs=pl.BlockSpec((rows, cols), lambda k: (0, 0)),
        scratch_shapes=[pltpu.VMEM((rows, cols), F32)] * 2,
        cost_estimate=pl.CostEstimate(
            flops=4 * rows * depth * cols,
            bytes_accessed=2 * depth * (rows + 2 * cols),
            transcendentals=0,
        ),
    )(x, w_gate, w_up)


def down_kernel(h_ref, d_ref, sh_ref, sd_ref, out_ref):
    slots = h_ref.shape[0]
    out_ref[0, 0:slots, :] = jnp.dot(h_ref[...], d_ref[...], preferred_element_type=F32).astype(BF16)
    out_ref[0, slots:, :] = jnp.dot(sh_ref[...], sd_ref[...], preferred_element_type=F32).astype(
        BF16
    )


def down_parts(hidden, w_down, shared_hidden, shared_down, blocks):
    slots, depth = hidden.shape
    shared_rows, shared_depth = shared_hidden.shape
    feat = w_down.shape[1] // blocks
    rows = slots + shared_rows
    return pl.pallas_call(
        down_kernel,
        grid=(blocks,),
        out_shape=jax.ShapeDtypeStruct((blocks, rows, feat), BF16),
        in_specs=[
            pl.BlockSpec((slots, depth), lambda j: (0, 0)),
            pl.BlockSpec((depth, feat), lambda j: (0, j)),
            pl.BlockSpec((shared_rows, shared_depth), lambda j: (0, 0)),
            pl.BlockSpec((shared_depth, feat), lambda j: (0, j)),
        ],
        out_specs=pl.BlockSpec((1, rows, feat), lambda j: (j, 0, 0)),
        cost_estimate=pl.CostEstimate(
            flops=2 * slots * depth * feat * blocks, bytes_accessed=10_000_000, transcendentals=0
        ),
    )(hidden, w_down, shared_hidden, shared_down)


def weight_columns(out_weight):
    tp_count, ep_count = lax.axis_size("tp"), lax.axis_size("ep")
    depth, features = out_weight.shape
    mine = features // tp_count
    share = mine // ep_count
    part = lax.dynamic_index_in_dim(
        out_weight.reshape(depth, tp_count, ep_count, share), lax.axis_index("ep"), 2, False
    )
    part = part.transpose(1, 0, 2)
    part = lax.all_to_all(part, "tp", split_axis=0, concat_axis=0, tiled=True)
    whole = lax.all_gather(part.reshape(tp_count * depth, share), "ep")
    return whole.transpose(1, 0, 2).reshape(tp_count * depth, mine)


def local(
    queries,
    keys,
    values,
    out_gate,
    in_gate,
    forget_gate,
    out_gain,
    out_weight,
    moe_rows,
    moe_gain,
    routes,
    route_weight,
    expert_gate,
    expert_up,
    expert_down,
    shared_gate,
    shared_up,
    shared_down,
):
    tp_count = lax.axis_size("tp")
    ep_count = lax.axis_size("ep")
    routed_rows, topk_count = routes.shape
    local_experts = expert_gate.shape[0]
    assert local_experts == 1
    expert_count = local_experts * ep_count
    capacity = 3 * routed_rows * topk_count // (2 * expert_count)
    slot_count = expert_count * capacity

    rows_wide = moe_rows.astype(F32)
    inverse = lax.rsqrt(jnp.mean(rows_wide * rows_wide, axis=1, keepdims=True) + 1e-06)
    normed = (rows_wide * inverse * moe_gain).astype(BF16)
    flat_routes = routes.reshape(-1)
    count = flat_routes.shape[0]
    onehot = flat_routes[:, None] == jnp.arange(expert_count, dtype=jnp.int32)[None, :]
    earlier = jnp.tril(jnp.ones((count, count), BF16), -1)
    before = jnp.dot(earlier, onehot.astype(BF16), preferred_element_type=F32)
    token_position = jnp.sum(jnp.where(onehot, before, 0.0), axis=1).astype(jnp.int32)
    destination = (flat_routes * capacity + token_position).reshape(routed_rows, topk_count)
    slots = jnp.arange(slot_count, dtype=jnp.int32)
    hit = destination[:, :, None] == slots[None, None, :]
    place = jnp.any(hit, axis=1).astype(BF16)
    outgoing = lax.dot_general(
        place, normed, (((0,), (0,)), ((), ())), preferred_element_type=F32
    ).astype(BF16)
    arrived = lax.all_to_all(outgoing, "ep", split_axis=0, concat_axis=0, tiled=True)

    out_columns = weight_columns(out_weight)
    mixed = mixed_cells(queries, keys, values, out_gate, in_gate, forget_gate, out_gain)
    gathered = lax.all_gather(mixed, "tp")

    shared_hidden = hidden_units(normed, shared_gate, shared_up)
    hidden = hidden_units(arrived, expert_gate[0], expert_up[0])
    parts = down_parts(hidden, expert_down[0], shared_hidden, shared_down, tp_count)
    total_rows = parts.shape[1]
    summed = lax.psum_scatter(
        parts.reshape(tp_count * total_rows, parts.shape[2]), "tp", scatter_dimension=0, tiled=True
    )
    returned = lax.all_to_all(summed[:slot_count], "ep", split_axis=0, concat_axis=0, tiled=True)
    weights = jnp.sum(jnp.where(hit, route_weight[:, :, None], 0.0), axis=1)
    picked = jnp.dot(
        weights, returned.astype(F32), precision=lax.Precision.HIGHEST, preferred_element_type=F32
    )
    moe_out = (picked + summed[slot_count:].astype(F32)).astype(BF16)
    mixer_out = mixer(gathered, out_columns)
    return (mixer_out, moe_out)


def solution(mesh):
    return jax.shard_map(
        local,
        mesh=mesh,
        in_specs=(
            P("ep", "tp"),
            P("ep", "tp"),
            P("ep", "tp"),
            P("ep", "tp"),
            P("tp", "ep"),
            P("tp", "ep"),
            P("tp"),
            P("tp", None),
            P("ep", None),
            P(),
            P("ep", None),
            P("ep", None),
            P("ep", None, "tp"),
            P("ep", None, "tp"),
            P("ep", "tp", None),
            P(None, "tp"),
            P(None, "tp"),
            P("tp", None),
        ),
        out_specs=(P("ep", "tp"), P("ep", "tp")),
        check_vma=False,
    )
```

```python
import functools

import jax
import jax.numpy as jnp
from jax import lax
from jax.experimental import pallas as pl
from jax.experimental.pallas import tpu as pltpu
from jax.sharding import PartitionSpec as P


DK = 64
DV = 128
CH = 128
F32 = jnp.float32
BF16 = jnp.bfloat16
VM = pl.BlockSpec(memory_space=pltpu.VMEM)


def gate_rows(ig, fg):
    lane = lax.broadcasted_iota(jnp.int32, ig.shape, 1)
    total = jnp.minimum(fg, 0.0) - jnp.log1p(jnp.exp(-jnp.abs(fg)))
    step = 1
    while step < CH:
        total = total + jnp.where(lane >= step, pltpu.roll(total, step, 1), 0.0)
        step *= 2
    level = ig - total
    top = level
    step = 1
    while step < CH:
        top = jnp.maximum(top, jnp.where(lane >= step, pltpu.roll(top, step, 1), -1e30))
        step *= 2
    return total, level, top


def columns_of(parts):
    rows = sum(part.shape[0] for part in parts)
    padded = -(-rows // 128) * 128
    if padded > rows:
        parts = list(parts) + [jnp.zeros((padded - rows, CH), F32)]
    return jnp.concatenate(parts, axis=0).T


def split_bf16(x):
    high = x.astype(BF16)
    return high, (x - high.astype(F32)).astype(BF16)


def weighted_keys(keys, cols, first, heads, chunks):
    lane_head = lax.broadcasted_iota(jnp.int32, keys.shape, 1) // DK
    weight = jnp.broadcast_to(cols[:, first : first + 1], keys.shape)
    for h in range(1, heads):
        at = first + h * chunks
        weight = jnp.where(lane_head == h, jnp.broadcast_to(cols[:, at : at + 1], keys.shape), weight)
    return split_bf16(keys.astype(F32) * weight)


def add_outer(kw, values):
    dims = (((0,), (0,)), ((), ()))
    return lax.dot_general(kw[0], values, dims, preferred_element_type=F32) + lax.dot_general(
        kw[1], values, dims, preferred_element_type=F32
    )


def pick_head(parts, shape, axis):
    head = lax.broadcasted_iota(jnp.int32, shape, axis) // DK
    out = jnp.broadcast_to(parts[0], shape)
    for h in range(1, len(parts)):
        out = jnp.where(head == h, jnp.broadcast_to(parts[h], shape), out)
    return out


def summary_kernel(heads, chunks, k_ref, v_ref, ig_ref, fg_ref, out_ref):
    width = heads * DK
    total, level, top = gate_rows(ig_ref[...], fg_ref[...])
    shape = total.shape
    chunk = lax.broadcasted_iota(jnp.int32, shape, 0) % chunks
    last = jnp.broadcast_to(total[:, CH - 1 : CH], shape)
    suffix = last
    step = 1
    while step < chunks:
        moved = pltpu.roll(suffix, shape[0] - step, 0)
        suffix = suffix + jnp.where(chunk + step < chunks, moved, 0.0)
        step *= 2
    reach = suffix + jnp.broadcast_to(top[:, CH - 1 : CH], shape)
    tops = [
        jnp.max(reach[h * chunks : (h + 1) * chunks], axis=0, keepdims=True) for h in range(heads)
    ]
    weight = [
        jnp.exp(
            level[h * chunks : (h + 1) * chunks] + suffix[h * chunks : (h + 1) * chunks] - tops[h]
        )
        for h in range(heads)
    ]
    cols = columns_of(weight)
    state = jnp.zeros((width, heads * DV + 128), F32)
    for c in range(chunks):
        rows = pl.ds(c * CH, CH)
        kw = weighted_keys(k_ref[rows, :], cols, c, heads, chunks)
        values = jnp.concatenate([v_ref[rows, :], jnp.ones((CH, 128), BF16)], axis=1)
        state = state + add_outer(kw, values)
    out_ref[...] = jnp.zeros_like(out_ref)
    out_ref[0:width, :] = pick_head(
        [state[:, h * DV : (h + 1) * DV] for h in range(heads)], (width, DV), 0
    )
    normal = state[:, heads * DV :].T
    out_ref[width : width + 1, 0:width] = normal[0:1, :]
    for h in range(heads):
        out_ref[width + 1 + h : width + 2 + h, :] = tops[h]
        at = width + 1 + heads + h
        out_ref[at : at + 1, :] = suffix[h * chunks : h * chunks + 1]


def cells_kernel(
    heads, chunks, pos_ref, q_ref, k_ref, v_ref, og_ref, ig_ref, fg_ref, gain_ref, sum_ref, out_ref
):
    width = heads * DK
    matrix = jnp.zeros((width, DV), F32)
    normal = jnp.zeros((1, width), F32)
    stab = [jnp.zeros((1, 128), F32) for _ in range(heads)]
    for e in range(sum_ref.shape[0]):
        reached = e < pos_ref[0]
        part = sum_ref.at[jnp.maximum(pos_ref[0] - 1 - e, 0)]
        old_w, new_w, new_stab = [], [], []
        for h in range(heads):
            at = width + 1 + h
            carried = part[at + heads : at + heads + 1, :] + stab[h]
            there = part[at : at + 1, :]
            joined = jnp.maximum(carried, there)
            old_w.append(jnp.where(reached, jnp.exp(carried - joined), 1.0))
            new_w.append(jnp.where(reached, jnp.exp(there - joined), 0.0))
            new_stab.append(jnp.where(reached, joined, stab[h]))
        matrix = (
            pick_head(old_w, (width, DV), 0) * matrix
            + pick_head(new_w, (width, DV), 0) * part[0:width, :]
        )
        normal = (
            pick_head([w[:, 0:width] for w in old_w], (1, width), 1) * normal
            + pick_head([w[:, 0:width] for w in new_w], (1, width), 1)
            * part[width : width + 1, 0:width]
        )
        stab = new_stab
    normal_cols = jnp.broadcast_to(normal, (128, width)).T
    state = jnp.concatenate([matrix] * heads + [normal_cols], axis=1)

    total, level, top = gate_rows(ig_ref[...], fg_ref[...])
    shape = total.shape
    last = jnp.broadcast_to(total[:, CH - 1 : CH], shape)
    last_top = jnp.broadcast_to(top[:, CH - 1 : CH], shape)
    entering, leaving = [], []
    for h in range(heads):
        now = stab[h]
        for c in range(chunks):
            r = h * chunks + c
            entering.append(now)
            now = last[r : r + 1] + jnp.maximum(now, last_top[r : r + 1])
            leaving.append(now)
    entering = jnp.concatenate(entering, axis=0)
    leaving = jnp.concatenate(leaving, axis=0)
    peak = jnp.maximum(top, entering)
    decay = jnp.exp(last + entering - leaving)
    count = heads * chunks
    cols = columns_of(
        [
            peak,
            jnp.exp(entering - peak),
            jnp.exp(-(total + peak)),
            jnp.exp(last + level - leaving),
        ]
    )
    causal = lax.broadcasted_iota(jnp.int32, (CH, CH), 0) >= lax.broadcasted_iota(
        jnp.int32, (CH, CH), 1
    )
    lane_head = lax.broadcasted_iota(jnp.int32, (CH, width), 1) // DK
    for c in range(chunks):
        rows = pl.ds(c * CH, CH)
        keys = k_ref[rows, :]
        values = v_ref[rows, :]
        queries = q_ref[rows, :] * jnp.asarray(DK**-0.5, BF16)
        high, low = split_bf16(state)
        for h in range(heads):
            r = h * chunks + c
            mine = jnp.where(lane_head == h, queries, jnp.zeros_like(queries))
            raw = lax.dot_general(
                mine, keys, (((1,), (1,)), ((), ())), preferred_element_type=F32
            )
            logs = level[r : r + 1, :] - cols[:, r : r + 1]
            scores = raw * jnp.exp(jnp.where(causal, logs, -jnp.inf))
            inner = jnp.dot(
                scores.astype(BF16), values[:, h * DV : (h + 1) * DV], preferred_element_type=F32
            )
            across = 0.0
            for piece in (high, low):
                rhs = jnp.concatenate(
                    [piece[:, h * DV : (h + 1) * DV], piece[:, heads * DV :]], axis=1
                )
                across = across + jnp.dot(mine, rhs, preferred_element_type=F32)
            inter = cols[:, count + r : count + r + 1]
            signed = jnp.sum(scores, axis=1, keepdims=True) + inter * across[:, DV : DV + 1]
            divisor = jnp.maximum(jnp.abs(signed), cols[:, 2 * count + r : 2 * count + r + 1])
            cells = (inner + inter * across[:, :DV]) * (1.0 / divisor)
            at = slice(h * DV, (h + 1) * DV)
            gate = og_ref[rows, at].astype(F32)
            out_ref[rows, at] = (cells / (1.0 + jnp.exp(-gate)) * gain_ref[:, at]).astype(BF16)
        if c + 1 < chunks:
            kw = weighted_keys(keys, cols, 3 * count + c, heads, chunks)
            scale = pick_head(
                [decay[h * chunks + c : h * chunks + c + 1] for h in range(heads)], (width, 128), 0
            )
            rhs = jnp.concatenate([values, jnp.ones((CH, 128), BF16)], axis=1)
            state = state * jnp.concatenate([scale] * (heads + 1), axis=1) + add_outer(kw, rhs)


def mixed_cells(queries, keys, values, out_gate, in_gate, forget_gate, out_gain):
    tok_rows = queries.shape[0]
    heads = in_gate.shape[0]
    chunks = tok_rows // CH
    width = heads * DK
    ig = in_gate.reshape(heads * chunks, CH)
    fg = forget_gate.reshape(heads * chunks, CH)
    extra = -(-(1 + 2 * heads) // 8) * 8
    summary = pl.pallas_call(
        functools.partial(summary_kernel, heads, chunks),
        out_shape=jax.ShapeDtypeStruct((width + extra, 128), F32),
        in_specs=[VM] * 4,
        out_specs=VM,
        cost_estimate=pl.CostEstimate(flops=400_000_000, bytes_accessed=8_000_000, transcendentals=0),
    )(keys, values, ig, fg)
    ep_count = lax.axis_size("ep")
    everything = jnp.stack(
        [
            lax.ppermute(summary, "ep", [(i, i + d) for i in range(ep_count - d)])
            for d in range(1, ep_count)
        ]
    )
    pos = lax.axis_index("ep").astype(jnp.int32).reshape(1)
    return pl.pallas_call(
        functools.partial(cells_kernel, heads, chunks),
        out_shape=jax.ShapeDtypeStruct((tok_rows, heads * DV), BF16),
        in_specs=[pl.BlockSpec(memory_space=pltpu.SMEM)] + [VM] * 8,
        out_specs=VM,
        cost_estimate=pl.CostEstimate(flops=2_000_000_000, bytes_accessed=16_000_000, transcendentals=0),
    )(pos, queries, keys, values, out_gate, ig, fg, out_gain.reshape(1, -1), everything)


def mixer_kernel(pos_ref, a_ref, w_ref, out_ref):
    parts, _, width = a_ref.shape
    total = jnp.dot(a_ref[pos_ref[0]], w_ref[0:width, :], preferred_element_type=F32)
    for d in range(1, parts):
        source = lax.rem(pos_ref[0] + parts - d, parts)
        total = total + jnp.dot(
            a_ref[source], w_ref[d * width : (d + 1) * width, :], preferred_element_type=F32
        )
    out_ref[...] = total.astype(out_ref.dtype)


def mixer(gathered, weight):
    parts, rows, width = gathered.shape
    cols = weight.shape[1]
    tile = min(256, rows)
    return pl.pallas_call(
        mixer_kernel,
        grid=(rows // tile,),
        out_shape=jax.ShapeDtypeStruct((rows, cols), BF16),
        in_specs=[
            pl.BlockSpec(memory_space=pltpu.SMEM),
            pl.BlockSpec((parts, tile, width), lambda r: (0, r, 0)),
            pl.BlockSpec((parts * width, cols), lambda r: (0, 0)),
        ],
        out_specs=pl.BlockSpec((tile, cols), lambda r: (r, 0)),
        cost_estimate=pl.CostEstimate(
            flops=2 * rows * parts * width * cols, bytes_accessed=8_000_000, transcendentals=0
        ),
    )(lax.axis_index("tp").astype(jnp.int32).reshape(1), gathered, weight)


def hidden_kernel(x_ref, g_ref, u_ref, out_ref, gate_acc, up_acc):
    k = pl.program_id(0)
    x = x_ref[...]
    gate = jnp.dot(x, g_ref[...], preferred_element_type=F32)
    up = jnp.dot(x, u_ref[...], preferred_element_type=F32)

    @pl.when(k == 0)
    def _():
        gate_acc[...] = gate
        up_acc[...] = up

    @pl.when(k > 0)
    def _():
        gate_acc[...] += gate
        up_acc[...] += up

    @pl.when(k == pl.num_programs(0) - 1)
    def _():
        g = gate_acc[...]
        out_ref[...] = (g / (1.0 + jnp.exp(-g)) * up_acc[...]).astype(BF16)


def hidden_units(x, w_gate, w_up):
    rows, depth = x.shape
    cols = w_gate.shape[1]
    tile = min(512, depth)
    return pl.pallas_call(
        hidden_kernel,
        grid=(depth // tile,),
        out_shape=jax.ShapeDtypeStruct((rows, cols), BF16),
        in_specs=[
            pl.BlockSpec((rows, tile), lambda k: (0, k)),
            pl.BlockSpec((tile, cols), lambda k: (k, 0)),
            pl.BlockSpec((tile, cols), lambda k: (k, 0)),
        ],
        out_specs=pl.BlockSpec((rows, cols), lambda k: (0, 0)),
        scratch_shapes=[pltpu.VMEM((rows, cols), F32)] * 2,
        cost_estimate=pl.CostEstimate(
            flops=4 * rows * depth * cols,
            bytes_accessed=2 * depth * (rows + 2 * cols),
            transcendentals=0,
        ),
    )(x, w_gate, w_up)


def down_kernel(h_ref, d_ref, sh_ref, sd_ref, out_ref):
    slots = h_ref.shape[0]
    out_ref[0, 0:slots, :] = jnp.dot(h_ref[...], d_ref[...], preferred_element_type=F32).astype(BF16)
    out_ref[0, slots:, :] = jnp.dot(sh_ref[...], sd_ref[...], preferred_element_type=F32).astype(
        BF16
    )


def down_parts(hidden, w_down, shared_hidden, shared_down, blocks):
    slots, depth = hidden.shape
    shared_rows, shared_depth = shared_hidden.shape
    feat = w_down.shape[1] // blocks
    rows = slots + shared_rows
    return pl.pallas_call(
        down_kernel,
        grid=(blocks,),
        out_shape=jax.ShapeDtypeStruct((blocks, rows, feat), BF16),
        in_specs=[
            pl.BlockSpec((slots, depth), lambda j: (0, 0)),
            pl.BlockSpec((depth, feat), lambda j: (0, j)),
            pl.BlockSpec((shared_rows, shared_depth), lambda j: (0, 0)),
            pl.BlockSpec((shared_depth, feat), lambda j: (0, j)),
        ],
        out_specs=pl.BlockSpec((1, rows, feat), lambda j: (j, 0, 0)),
        cost_estimate=pl.CostEstimate(
            flops=2 * slots * depth * feat * blocks, bytes_accessed=10_000_000, transcendentals=0
        ),
    )(hidden, w_down, shared_hidden, shared_down)


def weight_columns(out_weight):
    tp_count, ep_count = lax.axis_size("tp"), lax.axis_size("ep")
    depth, features = out_weight.shape
    mine = features // tp_count
    share = mine // ep_count
    me, turn = lax.axis_index("tp"), lax.axis_index("ep")

    def block(target):
        return lax.dynamic_slice_in_dim(out_weight, target * mine + turn * share, share, 1)

    received = [block(me)]
    for d in range(1, tp_count):
        received.append(
            lax.ppermute(
                block(lax.rem(me + d, tp_count)),
                "tp",
                [(i, (i + d) % tp_count) for i in range(tp_count)],
            )
        )
    part = jnp.concatenate(received, axis=0)
    whole = lax.all_gather(part, "ep")
    return whole.transpose(1, 0, 2).reshape(tp_count * depth, mine)


def local(
    queries,
    keys,
    values,
    out_gate,
    in_gate,
    forget_gate,
    out_gain,
    out_weight,
    moe_rows,
    moe_gain,
    routes,
    route_weight,
    expert_gate,
    expert_up,
    expert_down,
    shared_gate,
    shared_up,
    shared_down,
):
    tp_count = lax.axis_size("tp")
    ep_count = lax.axis_size("ep")
    routed_rows, topk_count = routes.shape
    local_experts = expert_gate.shape[0]
    assert local_experts == 1
    expert_count = local_experts * ep_count
    capacity = 3 * routed_rows * topk_count // (2 * expert_count)
    slot_count = expert_count * capacity

    rows_wide = moe_rows.astype(F32)
    inverse = lax.rsqrt(jnp.mean(rows_wide * rows_wide, axis=1, keepdims=True) + 1e-06)
    normed = (rows_wide * inverse * moe_gain).astype(BF16)
    flat_routes = routes.reshape(-1)
    count = flat_routes.shape[0]
    onehot = flat_routes[:, None] == jnp.arange(expert_count, dtype=jnp.int32)[None, :]
    earlier = jnp.tril(jnp.ones((count, count), BF16), -1)
    before = jnp.dot(earlier, onehot.astype(BF16), preferred_element_type=F32)
    token_position = jnp.sum(jnp.where(onehot, before, 0.0), axis=1).astype(jnp.int32)
    destination = (flat_routes * capacity + token_position).reshape(routed_rows, topk_count)
    slots = jnp.arange(slot_count, dtype=jnp.int32)
    hit = destination[:, :, None] == slots[None, None, :]
    place = jnp.any(hit, axis=1).astype(BF16)
    outgoing = lax.dot_general(
        place, normed, (((0,), (0,)), ((), ())), preferred_element_type=F32
    ).astype(BF16)
    arrived = lax.all_to_all(outgoing, "ep", split_axis=0, concat_axis=0, tiled=True)

    out_columns = weight_columns(out_weight)
    mixed = mixed_cells(queries, keys, values, out_gate, in_gate, forget_gate, out_gain)
    gathered = lax.all_gather(mixed, "tp")
    arrived, _ = lax.optimization_barrier((arrived, mixed))

    shared_hidden = hidden_units(normed, shared_gate, shared_up)
    hidden = hidden_units(arrived, expert_gate[0], expert_up[0])
    parts = down_parts(hidden, expert_down[0], shared_hidden, shared_down, tp_count)
    total_rows = parts.shape[1]
    summed = lax.psum_scatter(
        parts.reshape(tp_count * total_rows, parts.shape[2]),
        "tp",
        scatter_dimension=0,
        tiled=True,
    )
    returned = lax.all_to_all(summed[:slot_count], "ep", split_axis=0, concat_axis=0, tiled=True)
    weights = jnp.sum(jnp.where(hit, route_weight[:, :, None], 0.0), axis=1)
    picked = jnp.dot(
        weights, returned.astype(F32), precision=lax.Precision.HIGHEST, preferred_element_type=F32
    )
    moe_out = (picked + summed[slot_count:].astype(F32)).astype(BF16)
    mixer_out = mixer(gathered, out_columns)
    return (mixer_out, moe_out)


def solution(mesh):
    return jax.shard_map(
        local,
        mesh=mesh,
        in_specs=(
            P("ep", "tp"),
            P("ep", "tp"),
            P("ep", "tp"),
            P("ep", "tp"),
            P("tp", "ep"),
            P("tp", "ep"),
            P("tp"),
            P("tp", None),
            P("ep", None),
            P(),
            P("ep", None),
            P("ep", None),
            P("ep", None, "tp"),
            P("ep", None, "tp"),
            P("ep", "tp", None),
            P(None, "tp"),
            P(None, "tp"),
            P("tp", None),
        ),
        out_specs=(P("ep", "tp"), P("ep", "tp")),
        check_vma=False,
    )
```
